32 devices in a mesh: dp: 4 (over y, x), kv: 4 (over z), tp: 2 (over core).
Axes of the slice: x: 2, y: 2, z: 4, core: 2. Of those that a mesh axis runs over, the one named last changes fastest.
Arguments:
- tokens: bfloat16 [16, 4, 2048], P('dp', None, 'kv'), may hold values from -6 to 6
- in_gain: float32 [2048], P('kv'), may hold values from 0.1 to 1.9
- w_gate: bfloat16 [2048, 2048], P('kv', 'tp'), may hold values from -0.125 to 0.125
- w_value: bfloat16 [2048, 2048], P('kv', 'tp'), may hold values from -0.125 to 0.125
- w_key: bfloat16 [2048, 512], P('kv', 'tp'), may hold values from -0.125 to 0.125
- w_query: bfloat16 [2048, 512], P('kv', 'tp'), may hold values from -0.125 to 0.125
- w_step: bfloat16 [2048, 32], P('kv', 'tp'), may hold values from -0.125 to 0.125
- conv_value: bfloat16 [4, 2048], P(None, 'tp'), may hold values from -3 to 3
- conv_key: bfloat16 [4, 512], P(None, 'tp'), may hold values from -3 to 3
- conv_query: bfloat16 [4, 512], P(None, 'tp'), may hold values from -3 to 3
- step_bias: float32 [32], P('tp'), may hold values from -3 to 0
- decay_log: float32 [32], P('tp'), may hold values from -1 to 1.5
- out_gain: float32 [2048], P('tp'), may hold values from 0.1 to 1.9
- w_out: bfloat16 [2048, 2048], P('tp', 'kv'), may hold values from -0.125 to 0.125
- past_value: bfloat16 [16, 7, 2048], P(('dp', 'kv'), None, 'tp'), may hold values from -6 to 6
- past_key: bfloat16 [16, 7, 512], P(('dp', 'kv'), None, 'tp'), may hold values from -6 to 6
- past_query: bfloat16 [16, 7, 512], P(('dp', 'kv'), None, 'tp'), may hold values from -6 to 6
- past_states: float32 [16, 5, 32, 64, 128], P(('dp', 'kv'), None, 'tp'), may hold values from -2 to 2
- accepted: int32 [16], P(('dp', 'kv')), may hold values from 0 to 4
Outputs:
- mixed: bfloat16 [16, 4, 2048], P('dp', None, 'kv')
- new_states: float32 [16, 5, 32, 64, 128], P(('dp', 'kv'), None, 'tp')
- new_value: bfloat16 [16, 7, 2048], P(('dp', 'kv'), None, 'tp')
- new_key: bfloat16 [16, 7, 512], P(('dp', 'kv'), None, 'tp')
- new_query: bfloat16 [16, 7, 512], P(('dp', 'kv'), None, 'tp')
The draws below stay inside these ranges and needn't reach their ends.
All inputs are finite; a program needn't handle non-finite values.
Results may differ from the reference program's by a relative error of at most 0.014.
Values may be sent and summed in bfloat16 or wider, within the bound.
A program may use at most 64 MiB of HBM per device.

```python
import jax
import jax.numpy as jnp
from jax import lax

D = 2048
HEADS = 32
HEAD_DIM = 64
GROUPS = 4
STATE = 128
CONV = 4
PROP = 4
WIDTH = 2048
KEEP = 5
LAG = 7
SEQS = 16
N_TP = 2


def place_ends(values, key, low, largest):
    extent = values.shape
    index_at = [jax.random.randint(jax.random.fold_in(key, axis), (), 0, extent[axis]) for axis in range(len(extent))]
    values = values.at[tuple(index_at)].set(low)
    longest = extent.index(max(extent))
    index_at[longest] = (index_at[longest] + 1) % extent[longest]
    return values.at[tuple(index_at)].set(largest)


def steps_of(own_key, extent, cuts, least, high):
    factor_of = 1.0
    for dim, shards_of in cuts:
        heights = jax.random.uniform(jax.random.fold_in(jax.random.fold_in(own_key, 6), dim), (shards_of,), jnp.float32, least / len(cuts), high / len(cuts))
        factor_of = factor_of * jnp.repeat(jnp.exp(heights), extent[dim] // shards_of).reshape((-1,) + (1,) * (len(extent) - 1 - dim))
    return factor_of


def centred(rng, dims, deviation, reach, pieces=(), kind=jnp.bfloat16):
    array = deviation * jax.random.normal(rng, dims, jnp.float32)
    if pieces:
        array = array * steps_of(rng, dims, pieces, -0.22, 0.18)
    return jnp.clip(array, -reach, reach).astype(kind)


def setup_inputs(seed: int = 0) -> dict:
    splits = jax.random.split(jax.random.key(seed), 20)
    return {
        "tokens": centred(splits[0], (SEQS, PROP, D), 1.0, 6.0, ((0, 4), (2, 4))),
        "in_gain": jnp.clip(1.0 + 0.18 * jax.random.normal(splits[1], (D,), jnp.float32), 0.1, 1.9),
        "w_gate": centred(splits[2], (D, WIDTH), D ** -0.5, 0.125, ((0, 4), (1, 2))),
        "w_value": centred(splits[3], (D, WIDTH), D ** -0.5, 0.125, ((0, 4), (1, 2))),
        "w_key": centred(splits[4], (D, GROUPS * STATE), D ** -0.5, 0.125, ((0, 4), (1, 2))),
        "w_query": centred(splits[5], (D, GROUPS * STATE), D ** -0.5, 0.125, ((0, 4), (1, 2))),
        "w_step": centred(splits[6], (D, HEADS), D ** -0.5, 0.125, ((0, 4), (1, 2))),
        "conv_value": centred(splits[7], (CONV, WIDTH), 0.5, 3.0, ((1, 2),)),
        "conv_key": centred(splits[8], (CONV, GROUPS * STATE), 0.5, 3.0, ((1, 2),)),
        "conv_query": centred(splits[9], (CONV, GROUPS * STATE), 0.5, 3.0, ((1, 2),)),
        "step_bias": jnp.clip(-3.0 + 3.0 * jax.random.uniform(splits[10], (HEADS,), jnp.float32) ** steps_of(splits[10], (HEADS,), ((0, 2),), -0.2, 0.2), -3.0, 0.0),
        "decay_log": jnp.clip(-1.0 + 2.5 * jax.random.uniform(splits[11], (HEADS,), jnp.float32) ** steps_of(splits[11], (HEADS,), ((0, 2),), -0.2, 0.2), -1.0, 1.5),
        "out_gain": jnp.clip(1.0 + 0.18 * jax.random.normal(splits[12], (WIDTH,), jnp.float32), 0.1, 1.9),
        "w_out": centred(splits[13], (WIDTH, D), WIDTH ** -0.5, 0.125, ((0, 2), (1, 4))),
        "past_value": centred(splits[14], (SEQS, LAG, WIDTH), 1.0, 6.0, ((0, 16), (2, 2))),
        "past_key": centred(splits[15], (SEQS, LAG, GROUPS * STATE), 1.0, 6.0, ((0, 16), (2, 2))),
        "past_query": centred(splits[16], (SEQS, LAG, GROUPS * STATE), 1.0, 6.0, ((0, 16), (2, 2))),
        "past_states": centred(splits[17], (SEQS, KEEP, HEADS, HEAD_DIM, STATE), 0.3, 2.0, ((0, 16), (2, 2)), jnp.float32),
        "accepted": place_ends(jax.random.randint(splits[18], (SEQS,), 0, PROP + 1), jax.random.fold_in(splits[18], 1), 0, PROP).astype(jnp.int32),
    }


EPS = 1e-05

def take_window(history, offsets, span):
    return jax.vmap(lambda rows_one, offset: lax.dynamic_slice_in_dim(rows_one, offset, span, 0))(history, offsets.astype(jnp.int32))

def depthwise(history, taps, proposals):
    total = history[:, 0:proposals].astype(jnp.float32) * taps[0].astype(jnp.float32)
    for offset in range(1, taps.shape[0]):
        total = total + history[:, offset:offset + proposals].astype(jnp.float32) * taps[offset].astype(jnp.float32)
    return jax.nn.silu(total)

def run_chain(values, keys, queries, steps, rates, initial, groups):
    seq_count, proposals, heads = steps.shape
    per_group = heads // groups
    head_dim = values.shape[2] // heads
    state_dim = keys.shape[2] // groups
    carried = initial.reshape(seq_count, groups, per_group, head_dim, state_dim)
    factor = jnp.exp(steps * rates)
    outputs = []
    saved = [initial]
    for position in range(proposals):
        moved = values[:, position].reshape(seq_count, groups, per_group, head_dim) * steps[:, position].reshape(seq_count, groups, per_group)[..., None]
        key_row = keys[:, position].reshape(seq_count, groups, state_dim)
        carried = carried * factor[:, position].reshape(seq_count, groups, per_group)[..., None, None] + moved[..., None] * key_row[:, :, None, None, :]
        query_row = queries[:, position].reshape(seq_count, groups, state_dim)
        result = jnp.einsum('sgrpn,sgn->sgrp', carried, query_row, precision=lax.Precision.HIGHEST)
        outputs.append(result.reshape(seq_count, heads * head_dim))
        saved.append(carried.reshape(seq_count, heads, head_dim, state_dim))
    return (jnp.stack(outputs, 1), jnp.stack(saved, 1))

def reference(tokens, in_gain, w_gate, w_value, w_key, w_query, w_step, conv_value, conv_key, conv_query, step_bias, decay_log, out_gain, w_out, past_value, past_key, past_query, past_states, accepted):
    seq_count, proposals, features = tokens.shape
    widened = tokens.astype(jnp.float32)
    rscale = lax.rsqrt(lax.optimization_barrier(jnp.mean(widened * widened, axis=-1, keepdims=True)) + EPS)
    normed = (widened * in_gain).astype(jnp.bfloat16).reshape(seq_count * proposals, features)

    def project(weight):
        return jnp.dot(normed, weight, preferred_element_type=jnp.float32).reshape(seq_count, proposals, -1) * rscale
    raw_step = project(w_step)
    gate = project(w_gate).astype(jnp.bfloat16)
    value = project(w_value).astype(jnp.bfloat16)
    key = project(w_key).astype(jnp.bfloat16)
    query = project(w_query).astype(jnp.bfloat16)
    span = CONV - 1
    new_value = jnp.concatenate([take_window(past_value, accepted, span), value], axis=1)
    new_key = jnp.concatenate([take_window(past_key, accepted, span), key], axis=1)
    new_query = jnp.concatenate([take_window(past_query, accepted, span), query], axis=1)
    conv_v = depthwise(new_value, conv_value, proposals)
    conv_k = depthwise(new_key, conv_key, proposals)
    conv_q = depthwise(new_query, conv_query, proposals)
    steps = jax.nn.softplus(raw_step + step_bias)
    rates = -jnp.exp(decay_log)
    initial = jnp.take_along_axis(past_states, accepted.astype(jnp.int32)[:, None, None, None, None], axis=1)[:, 0]
    mixed_heads, new_states = run_chain(conv_v, conv_k, conv_q, steps, rates, initial, GROUPS)
    gated = mixed_heads * jax.nn.silu(gate.astype(jnp.float32))
    scale_out = lax.rsqrt(lax.optimization_barrier(jnp.mean(gated * gated, axis=-1, keepdims=True)) + EPS)
    outn = (gated * scale_out * out_gain).astype(jnp.bfloat16).reshape(seq_count * proposals, -1)
    block_width = outn.shape[1] // N_TP
    total = jnp.zeros((seq_count * proposals, features), jnp.float32)
    for block_index in range(N_TP):
        piece = outn[:, block_index * block_width:(block_index + 1) * block_width]
        weight_rows = w_out[block_index * block_width:(block_index + 1) * block_width]
        partial_sum = jnp.dot(piece, weight_rows, preferred_element_type=jnp.float32).astype(jnp.bfloat16)
        total = total + partial_sum.astype(jnp.float32)
    mixed = total.astype(jnp.bfloat16).reshape(seq_count, proposals, features)
    return (mixed, new_states, new_value, new_key, new_query)
```

```python
import functools

import jax
import jax.numpy as jnp
from jax import lax
from jax.experimental import pallas as pl
from jax.experimental.pallas import tpu as pltpu
from jax.sharding import PartitionSpec as P

STATE = 128
EPS = 1e-05
LANES = 128
MESH = pl.DeviceIdType.MESH
F32 = jnp.float32
BF16 = jnp.bfloat16
COMMON = (((1,), (1,)), ((), ()))


def parts_of(x, count):
    found = []
    for _ in range(count):
        piece = x.astype(BF16)
        found.append(piece)
        x = x - piece.astype(F32)
    return found


def silu(x):
    return x / (1.0 + jnp.exp(-x))


def dot(a, b):
    return jnp.dot(a, b, preferred_element_type=F32)


def mixer_kernel(n_kv, n_tp, *refs):
    (tok_h, gain_h, wg_h, wv_h, wk_h, wq_h, ws_h, cv_h, ck_h, cq_h, bias_h, dlog_h, ogain_h, wo_h,
     pv_h, pk_h, pq_h, states_h, acc_ref,
     mixed_ref, hist_ref, aux_ref, convk_ref,
     tok, gain, wg, wv, wk, wq, ws, cv, ck, cq, bias, dlog, ogain, wo, pv, pk, pq, states,
     rows_f, send1, recv1, own1, send2, recv2, own2, expand, shi, slo, gbuf, rows_g, psend, precv,
     load_sem, s1, r1, s2, r2, s3, r3, s4, r4) = refs
    kv = lax.axis_index("kv")
    tp = lax.axis_index("tp")
    n_seq, prop, feat = tok.shape
    own = pv.shape[0]
    rows = n_seq * prop
    width, kwidth, heads = wv.shape[1], wk.shape[1], ws.shape[1]
    head_dim = width // heads
    groups = kwidth // STATE
    gwidth = width // groups
    taps = cv.shape[0]
    cols = wo.shape[1]
    pcols = psend.shape[1] - 2 * LANES
    conv_cols = width + 2 * kwidth

    barrier = pltpu.get_barrier_semaphore()
    for d in range(1, n_kv):
        pl.semaphore_signal(barrier, inc=1, device_id={"kv": lax.rem(kv + d, n_kv)}, device_id_type=MESH)
    for d in range(1, n_tp):
        pl.semaphore_signal(barrier, inc=1, device_id={"tp": lax.rem(tp + d, n_tp)}, device_id_type=MESH)

    pairs = dict(
        tok=(tok_h, tok), gain=(gain_h, gain), ws=(ws_h, ws), wk=(wk_h, wk), wq=(wq_h, wq), wv=(wv_h, wv),
        wg=(wg_h, wg), pv=(pv_h, pv), pk=(pk_h, pk), pq=(pq_h, pq), cv=(cv_h, cv), ck=(ck_h, ck), cq=(cq_h, cq),
        bias=(bias_h, bias), dlog=(dlog_h, dlog), ogain=(ogain_h, ogain), states=(states_h, states), wo=(wo_h, wo),
    )
    loads = {}
    for place, (name, (src, dst)) in enumerate(pairs.items()):
        loads[name] = pltpu.make_async_copy(src, dst, load_sem.at[place])
        loads[name].start()

    row_at = lax.broadcasted_iota(jnp.int32, (LANES, width), 0)
    col_at = lax.broadcasted_iota(jnp.int32, (LANES, width), 1)
    expand[...] = jnp.where(row_at == col_at // head_dim, 1.0, 0.0).astype(BF16)
    lane = lax.broadcasted_iota(jnp.int32, (rows, LANES), 1)

    loads["tok"].wait()
    loads["gain"].wait()
    for s in range(n_seq):
        rows_f[s * prop:(s + 1) * prop, :] = tok[s].astype(F32)
    x = rows_f[...]
    normed = (x * gain[...].reshape(1, feat)).astype(BF16)
    squares = jnp.sum(x * x, axis=1, keepdims=True)

    def stage(product, send, kept, at):
        n = product.shape[1]
        for s in range(n_seq):
            piece = product[s * prop:(s + 1) * prop]
            kept[s, :, at:at + n] = piece
            send[s, :, at:at + n] = piece.astype(BF16)

    loads["ws"].wait()
    step_part = dot(normed, ws[...])
    rows_g[:, 0:LANES] = jnp.zeros((rows, LANES), F32)
    rows_g[:, 0:heads] = step_part
    stat = jnp.where(lane == heads, squares, rows_g[:, 0:LANES])
    stat_hi, stat_lo = parts_of(stat, 2)
    for s in range(n_seq):
        own1[s, :, conv_cols:conv_cols + LANES] = stat[s * prop:(s + 1) * prop]
        send1[s, :, conv_cols:conv_cols + LANES] = stat_hi.astype(F32)[s * prop:(s + 1) * prop].astype(BF16)
        send1[s, :, conv_cols + LANES:] = stat_lo.astype(F32)[s * prop:(s + 1) * prop].astype(BF16)
    loads["wk"].wait()
    stage(dot(normed, wk[...]), send1, own1, width)
    loads["wq"].wait()
    stage(dot(normed, wq[...]), send1, own1, width + kwidth)
    loads["wv"].wait()
    stage(dot(normed, wv[...]), send1, own1, 0)

    pl.semaphore_wait(barrier, n_kv - 1 + n_tp - 1)

    def scatter(send, recv, send_sem, recv_sem):
        copies = []
        for d in range(1, n_kv):
            peer = lax.rem(kv + d, n_kv)
            copies.append(pltpu.make_async_remote_copy(
                src_ref=send.at[pl.ds(peer * own, own)], dst_ref=recv.at[d - 1],
                send_sem=send_sem.at[d - 1], recv_sem=recv_sem.at[d - 1],
                device_id={"kv": peer}, device_id_type=MESH))
        order = sorted(range(n_kv - 1), key=lambda i: -min(i + 1, n_kv - 1 - i))
        for i in order:
            copies[i].start()
        return copies

    first = scatter(send1, recv1, s1, r1)
    loads["wg"].wait()
    stage(dot(normed, wg[...]), send2, own2, 0)
    second = scatter(send2, recv2, s2, r2)

    for name in ("pv", "pk", "pq", "cv", "ck", "cq", "bias", "dlog", "ogain"):
        loads[name].wait()
    span = taps - 1
    for j in range(own):
        chosen = acc_ref[j]
        at = 0
        for past in (pv, pk, pq):
            wide = past[j].astype(F32)
            window = wide[0:span]
            for a in range(1, wide.shape[0] - span + 1):
                window = jnp.where(chosen == a, wide[a:a + span], window)
            hist_ref[j, 0:span, at:at + wide.shape[1]] = window
            at += wide.shape[1]
    rate = -jnp.exp(dlog[...].reshape(1, heads))
    each = lax.broadcasted_iota(jnp.int32, (8, heads), 0)
    known = jnp.where(each == 0, bias[...].reshape(1, heads), jnp.where(each == 1, rate, 0.0))
    spread = sum(dot(piece, expand[0:heads, :]) for piece in parts_of(known, 3))
    bias_e, rate_e = spread[0:1], spread[1:2]
    taps_v, taps_k, taps_q = (c[...].astype(F32) for c in (cv, ck, cq))
    gain_out = ogain[...].reshape(1, width)
    loads["states"].wait()
    for j in range(own):
        start = states[j, acc_ref[j]].reshape(width, STATE)
        hi, lo = parts_of(start, 2)
        shi[j] = hi
        slo[j] = lo

    for copy in first:
        copy.wait()
    t_at = lax.broadcasted_iota(jnp.int32, (prop, width), 0)
    results = []
    for j in range(own):
        mine = kv * own + j
        total = own1[mine]
        sums = total[:, 0:conv_cols]
        stats = total[:, conv_cols:conv_cols + LANES]
        for d in range(n_kv - 1):
            got = recv1[d, j].astype(F32)
            sums = sums + got[:, 0:conv_cols]
            stats = stats + got[:, conv_cols:conv_cols + LANES] + got[:, conv_cols + LANES:]
        rscale = lax.rsqrt(stats[:, heads:heads + 1] / (feat * n_kv) + EPS)
        raw = stats[:, 0:heads] * rscale
        raw_e = sum(dot(piece, expand[0:heads, :]) for piece in parts_of(raw, 3))
        hist_ref[j, span:span + prop, :] = (sums * rscale).astype(BF16).astype(F32)

        def conv(c, at, n):
            total = hist_ref[j, 0:prop, at:at + n] * c[0:1]
            for i in range(1, taps):
                total = total + hist_ref[j, i:i + prop, at:at + n] * c[i:i + 1]
            return silu(total)

        conv_k = conv(taps_k, width, kwidth)
        conv_q = conv(taps_q, width + kwidth, kwidth)
        conv_v = conv(taps_v, 0, width)
        pre = raw_e + bias_e
        dt = jnp.maximum(pre, 0.0) + jnp.log1p(jnp.exp(-jnp.abs(pre)))
        logd = dt * rate_e
        moved = dt * conv_v
        aux_ref[j, 0:prop, :] = moved
        aux_ref[j, prop:2 * prop, :] = jnp.exp(logd)
        convk_ref[j] = conv_k
        cum = jnp.zeros_like(logd)
        for s in range(prop):
            cum = cum + jnp.where(t_at >= s, logd[s:s + 1], 0.0)
        parts = []
        for g in range(groups):
            qg = conv_q[:, g * STATE:(g + 1) * STATE]
            kg = conv_k[:, g * STATE:(g + 1) * STATE]
            q_hi, q_lo = parts_of(qg, 2)
            s_hi = shi[j, g * gwidth:(g + 1) * gwidth, :]
            s_lo = slo[j, g * gwidth:(g + 1) * gwidth, :]
            read = functools.partial(lax.dot_general, dimension_numbers=COMMON, preferred_element_type=F32)
            y = read(q_hi, s_hi) + read(q_lo, s_hi) + read(q_hi, s_lo)
            lo_at = g * gwidth
            cum_g = cum[:, lo_at:lo_at + gwidth]
            y = y * jnp.exp(cum_g)
            for s in range(prop):
                kq = jnp.sum(qg * kg[s:s + 1], axis=1, keepdims=True)
                weight = jnp.exp(jnp.where(t_at[:, 0:gwidth] >= s, cum_g - cum_g[s:s + 1], -jnp.inf))
                y = y + weight * (moved[s:s + 1, lo_at:lo_at + gwidth] * kq)
            parts.append(y)
        results.append((jnp.concatenate(parts, axis=1), rscale))

    for copy in second:
        copy.wait()
    for j in range(own):
        mine = kv * own + j
        y, rscale = results[j]
        total = own2[mine]
        for d in range(n_kv - 1):
            total = total + recv2[d, j].astype(F32)
        gate = (total * rscale).astype(BF16).astype(F32)
        gated = y * silu(gate)
        sq_hi, sq_lo = parts_of(jnp.broadcast_to(jnp.sum(gated * gated, axis=1, keepdims=True), (prop, LANES)), 2)
        gbuf[mine, :, 0:width] = (gated * gain_out).astype(BF16)
        gbuf[mine, :, width:width + LANES] = sq_hi
        gbuf[mine, :, width + LANES:] = sq_lo

    gathers = []
    for d in range(1, n_kv):
        peer = lax.rem(kv + d, n_kv)
        gathers.append(pltpu.make_async_remote_copy(
            src_ref=gbuf.at[pl.ds(kv * own, own)], dst_ref=gbuf.at[pl.ds(kv * own, own)],
            send_sem=s3.at[d - 1], recv_sem=r3.at[d - 1],
            device_id={"kv": peer}, device_id_type=MESH))
    for i in sorted(range(n_kv - 1), key=lambda i: -min(i + 1, n_kv - 1 - i)):
        gathers[i].start()
    loads["wo"].wait()
    for i, copy in enumerate(gathers):
        copy.wait()
    for s in range(n_seq):
        rows_g[s * prop:(s + 1) * prop, :] = gbuf[s].astype(F32)
    outn = rows_g[:, 0:width].astype(BF16)
    psend[:, 0:cols] = dot(outn, wo[...]).astype(BF16)
    psend[:, pcols:pcols + LANES] = rows_g[:, width:width + LANES].astype(BF16)
    psend[:, pcols + LANES:] = rows_g[:, width + LANES:].astype(BF16)
    swaps = []
    for d in range(1, n_tp):
        swaps.append(pltpu.make_async_remote_copy(
            src_ref=psend, dst_ref=precv.at[d - 1], send_sem=s4.at[d - 1], recv_sem=r4.at[d - 1],
            device_id={"tp": lax.rem(tp + d, n_tp)}, device_id_type=MESH))
        swaps[-1].start()
    total = psend[:, 0:cols].astype(F32)
    square = rows_g[:, width:width + 1] + rows_g[:, width + LANES:width + LANES + 1]
    for d, copy in enumerate(swaps):
        copy.wait()
        total = total + precv[d, :, 0:cols].astype(F32)
        square = square + precv[d, :, pcols:pcols + 1].astype(F32)
        square = square + precv[d, :, pcols + LANES:pcols + LANES + 1].astype(F32)
    mixed = total * lax.rsqrt(square / (width * n_tp) + EPS)
    for s in range(n_seq):
        mixed_ref[s] = mixed[s * prop:(s + 1) * prop].astype(BF16)


def states_kernel(chunk, mixed_in, hist, aux, convk, states_h, acc_ref,
                  mixed_ref, new_h, nv_ref, nk_ref, nq_ref, buf, cols_t, in_sem, out_sem):
    own, keep, heads, head_dim, state = buf.shape
    steps = keep - 1
    per_group = heads // (convk.shape[2] // state)
    chunks = heads // chunk
    loads = [[pltpu.make_async_copy(
        states_h.at[j, acc_ref[j], pl.ds(c * chunk, chunk)], buf.at[j, 0, pl.ds(c * chunk, chunk)],
        in_sem.at[j, c]) for c in range(chunks)] for j in range(own)]
    for j in range(own):
        for c in range(chunks):
            loads[j][c].start()
    mixed_ref[...] = mixed_in[...]
    at = 0
    for ref in (nv_ref, nk_ref, nq_ref):
        n = ref.shape[2]
        for j in range(own):
            ref[j] = hist[j, 0:ref.shape[1], at:at + n].astype(BF16)
        at += n
    stores = []
    for j in range(own):
        cols_t[...] = jnp.transpose(aux[j])
        for c in range(chunks):
            loads[j][c].wait()
            for h in range(c * chunk, (c + 1) * chunk):
                s = buf[j, 0, h]
                g = h // per_group
                for t in range(steps):
                    lift = cols_t[h * head_dim:(h + 1) * head_dim, t:t + 1]
                    fade = cols_t[h * head_dim:(h + 1) * head_dim, steps + t:steps + t + 1]
                    s = s * fade + lift * convk[j, t:t + 1, g * state:(g + 1) * state]
                    buf[j, t + 1, h] = s
            out = pltpu.make_async_copy(
                buf.at[j, :, pl.ds(c * chunk, chunk)], new_h.at[j, :, pl.ds(c * chunk, chunk)], out_sem.at[j, c])
            out.start()
            stores.append(out)
    for out in stores:
        out.wait()


def per_device(n_kv, n_tp, *args):
    (tokens, in_gain, w_gate, w_value, w_key, w_query, w_step, conv_value, conv_key, conv_query, step_bias,
     decay_log, out_gain, w_out, past_value, past_key, past_query, past_states, accepted) = args
    n_seq, prop, feat = tokens.shape
    own, keep, heads, head_dim, state = past_states.shape
    width, kwidth, cols = w_value.shape[1], w_key.shape[1], w_out.shape[1]
    conv_cols = width + 2 * kwidth
    wide1 = conv_cols + 2 * LANES
    gcols = width + 2 * LANES
    pcols = -(-cols // LANES) * LANES + 2 * LANES
    rows = n_seq * prop
    hist_rows = past_value.shape[1]
    vmem = pl.BlockSpec(memory_space=pltpu.VMEM)
    anywhere = pl.BlockSpec(memory_space=pl.ANY)
    smem = pl.BlockSpec(memory_space=pltpu.SMEM)
    dma = pltpu.SemaphoreType.DMA
    held = [pltpu.VMEM(a.shape, a.dtype) for a in args[:-1]]
    peers = n_kv - 1
    mixed, hist, aux, convk = pl.pallas_call(
        functools.partial(mixer_kernel, n_kv, n_tp),
        out_shape=(
            jax.ShapeDtypeStruct((n_seq, prop, cols), BF16),
            jax.ShapeDtypeStruct((own, hist_rows, conv_cols), F32),
            jax.ShapeDtypeStruct((own, 2 * prop, width), F32),
            jax.ShapeDtypeStruct((own, prop, kwidth), F32),
        ),
        in_specs=[anywhere] * 18 + [smem],
        out_specs=(vmem,) * 4,
        scratch_shapes=held + [
            pltpu.VMEM((rows, feat), F32),
            pltpu.VMEM((n_seq, prop, wide1), BF16),
            pltpu.VMEM((peers, own, prop, wide1), BF16),
            pltpu.VMEM((n_seq, prop, conv_cols + LANES), F32),
            pltpu.VMEM((n_seq, prop, width), BF16),
            pltpu.VMEM((peers, own, prop, width), BF16),
            pltpu.VMEM((n_seq, prop, width), F32),
            pltpu.VMEM((LANES, width), BF16),
            pltpu.VMEM((own, width, state), BF16),
            pltpu.VMEM((own, width, state), BF16),
            pltpu.VMEM((n_seq, prop, gcols), BF16),
            pltpu.VMEM((rows, gcols), F32),
            pltpu.VMEM((rows, pcols), BF16),
            pltpu.VMEM((n_tp - 1, rows, pcols), BF16),
            dma((18,)),
            dma((peers,)), dma((peers,)), dma((peers,)), dma((peers,)), dma((peers,)), dma((peers,)),
            dma((n_tp - 1,)), dma((n_tp - 1,)),
        ],
        compiler_params=pltpu.CompilerParams(
            collective_id=0, has_side_effects=True, vmem_limit_bytes=24 * 1024 * 1024),
        name="mixer",
    )(*args)
    chunk = 4 if heads % 4 == 0 else 1
    mixed, new_states, new_value, new_key, new_query = pl.pallas_call(
        functools.partial(states_kernel, chunk),
        out_shape=(
            jax.ShapeDtypeStruct((n_seq, prop, cols), BF16),
            jax.ShapeDtypeStruct(past_states.shape, F32),
            jax.ShapeDtypeStruct(past_value.shape, BF16),
            jax.ShapeDtypeStruct(past_key.shape, BF16),
            jax.ShapeDtypeStruct(past_query.shape, BF16),
        ),
        in_specs=[vmem] * 4 + [anywhere, smem],
        out_specs=(vmem, anywhere, vmem, vmem, vmem),
        scratch_shapes=[
            pltpu.VMEM(past_states.shape, F32),
            pltpu.VMEM((width, 2 * prop), F32),
            dma((own, heads // chunk)), dma((own, heads // chunk)),
        ],
        compiler_params=pltpu.CompilerParams(vmem_limit_bytes=16 * 1024 * 1024),
        name="states",
    )(mixed, hist, aux, convk, past_states, accepted)
    return (mixed, new_states, new_value, new_key, new_query)


def solution(mesh):
    seqs = ("dp", "kv")
    placed = (
        P("dp", None, "kv"), P("kv"),
        P("kv", "tp"), P("kv", "tp"), P("kv", "tp"), P("kv", "tp"), P("kv", "tp"),
        P(None, "tp"), P(None, "tp"), P(None, "tp"),
        P("tp"), P("tp"), P("tp"), P("tp", "kv"),
        P(seqs, None, "tp"), P(seqs, None, "tp"), P(seqs, None, "tp"),
        P(seqs, None, "tp", None, None), P(seqs),
    )
    return jax.shard_map(
        functools.partial(per_device, mesh.shape["kv"], mesh.shape["tp"]),
        mesh=mesh,
        in_specs=placed,
        out_specs=(
            P("dp", None, "kv"),
            P(seqs, None, "tp", None, None),
            P(seqs, None, "tp"), P(seqs, None, "tp"), P(seqs, None, "tp"),
        ),
        check_vma=False,
    )
```

```python
import functools

import jax
import jax.numpy as jnp
from jax import lax
from jax.experimental import pallas as pl
from jax.experimental.pallas import tpu as pltpu
from jax.sharding import PartitionSpec as P

STATE = 128
EPS = 1e-05
LANES = 128
VMEM_BYTES = 67043328
MESH = pl.DeviceIdType.MESH
F32 = jnp.float32
BF16 = jnp.bfloat16
COMMON = (((1,), (1,)), ((), ()))


def parts_of(x, count):
    found = []
    for _ in range(count):
        piece = x.astype(BF16)
        found.append(piece)
        x = x - piece.astype(F32)
    return found


def silu(x):
    return x / (1.0 + jnp.exp(-x))


def dot(a, b):
    return jnp.dot(a, b, preferred_element_type=F32)


def mixer_kernel(n_kv, n_tp, *refs):
    (tok_h, gain_h, wg_h, wv_h, wk_h, wq_h, ws_h, cv_h, ck_h, cq_h, bias_h, dlog_h, ogain_h, wo_h,
     pv_h, pk_h, pq_h, states_h, acc_h,
     mixed_ref, hist_h, chain_h, convk_h, start_h,
     tok, gain, wg, wv, wk, wq, ws, cv, ck, cq, bias, dlog, ogain, wo, pv, pk, pq, states, acc_ref,
     rows_f, send1, recv1, own1, send2, recv2, own2, expand, shi, slo, gbuf, rows_g, psend, precv, hist_ref, chain, convk, start_v,
     load_sem, out_sem, s1, r1, s2, r2, s3, r3, s4, r4) = refs
    kv = lax.axis_index("kv")
    tp = lax.axis_index("tp")
    n_seq, prop, feat = tok.shape
    own = pv.shape[0]
    rows = n_seq * prop
    width, kwidth, heads = wv.shape[1], wk.shape[1], ws.shape[0]
    head_dim = width // heads
    groups = kwidth // STATE
    gwidth = width // groups
    taps = cv.shape[0]
    cols = wo.shape[1]
    pcols = psend.shape[1] - 2 * LANES
    conv_cols = width + 2 * kwidth

    barrier = pltpu.get_barrier_semaphore()
    for d in range(1, n_kv):
        pl.semaphore_signal(barrier, inc=1, device_id={"kv": lax.rem(kv + d, n_kv)}, device_id_type=MESH)
    for d in range(1, n_tp):
        pl.semaphore_signal(barrier, inc=1, device_id={"tp": lax.rem(tp + d, n_tp)}, device_id_type=MESH)

    pairs = dict(
        tok=(tok_h, tok), gain=(gain_h, gain), ws=(ws_h, ws), wk=(wk_h, wk), wq=(wq_h, wq), wv=(wv_h, wv),
        wg=(wg_h, wg), pv=(pv_h, pv), pk=(pk_h, pk), pq=(pq_h, pq), cv=(cv_h, cv), ck=(ck_h, ck), cq=(cq_h, cq),
        bias=(bias_h, bias), dlog=(dlog_h, dlog), ogain=(ogain_h, ogain), states=(states_h, states), wo=(wo_h, wo), acc=(acc_h, acc_ref),
    )
    loads = {}
    for place, (name, (src, dst)) in enumerate(pairs.items()):
        loads[name] = pltpu.make_async_copy(src, dst, load_sem.at[place])
        loads[name].start()

    row_at = lax.broadcasted_iota(jnp.int32, (LANES, width), 0)
    col_at = lax.broadcasted_iota(jnp.int32, (LANES, width), 1)
    expand[...] = jnp.where(row_at == col_at // head_dim, 1.0, 0.0).astype(BF16)
    lane = lax.broadcasted_iota(jnp.int32, (rows, LANES), 1)

    loads["tok"].wait()
    loads["gain"].wait()
    for s in range(n_seq):
        rows_f[s * prop:(s + 1) * prop, :] = tok[s].astype(F32)
    x = rows_f[...]
    normed = (x * gain[...].reshape(1, feat)).astype(BF16)
    squares = jnp.sum(x * x, axis=1, keepdims=True)

    def stage(product, send, kept, at):
        n = product.shape[1]
        for s in range(n_seq):
            piece = product[s * prop:(s + 1) * prop]
            kept[s, :, at:at + n] = piece
            send[s, :, at:at + n] = piece.astype(BF16)

    loads["ws"].wait()
    step_part = lax.dot_general(normed, ws[...], COMMON, preferred_element_type=F32)
    rows_g[:, 0:LANES] = jnp.zeros((rows, LANES), F32)
    rows_g[:, 0:heads] = step_part
    stat = jnp.where(lane == heads, squares, rows_g[:, 0:LANES])
    stat_hi, stat_lo = parts_of(stat, 2)
    for s in range(n_seq):
        own1[s, :, conv_cols:conv_cols + LANES] = stat[s * prop:(s + 1) * prop]
        send1[s, :, conv_cols:conv_cols + LANES] = stat_hi.astype(F32)[s * prop:(s + 1) * prop].astype(BF16)
        send1[s, :, conv_cols + LANES:] = stat_lo.astype(F32)[s * prop:(s + 1) * prop].astype(BF16)
    loads["wk"].wait()
    stage(dot(normed, wk[...]), send1, own1, width)
    loads["wq"].wait()
    stage(dot(normed, wq[...]), send1, own1, width + kwidth)
    loads["wv"].wait()
    stage(dot(normed, wv[...]), send1, own1, 0)

    pl.semaphore_wait(barrier, n_kv - 1 + n_tp - 1)

    def scatter(send, recv, send_sem, recv_sem):
        copies = []
        for d in range(1, n_kv):
            peer = lax.rem(kv + d, n_kv)
            copies.append(pltpu.make_async_remote_copy(
                src_ref=send.at[pl.ds(peer * own, own)], dst_ref=recv.at[d - 1],
                send_sem=send_sem.at[d - 1], recv_sem=recv_sem.at[d - 1],
                device_id={"kv": peer}, device_id_type=MESH))
        order = sorted(range(n_kv - 1), key=lambda i: -min(i + 1, n_kv - 1 - i))
        for i in order:
            copies[i].start()
        return copies

    first = scatter(send1, recv1, s1, r1)
    loads["wg"].wait()
    stage(dot(normed, wg[...]), send2, own2, 0)
    second = scatter(send2, recv2, s2, r2)

    for name in ("acc", "pv", "pk", "pq", "cv", "ck", "cq", "bias", "dlog", "ogain"):
        loads[name].wait()
    span = taps - 1
    for j in range(own):
        chosen = acc_ref[j]
        at = 0
        for past in (pv, pk, pq):
            wide = past[j].astype(F32)
            window = wide[0:span]
            for a in range(1, wide.shape[0] - span + 1):
                window = jnp.where(chosen == a, wide[a:a + span], window)
            hist_ref[j, 0:span, at:at + wide.shape[1]] = window
            at += wide.shape[1]
    rate = -jnp.exp(dlog[...].reshape(1, heads))
    each = lax.broadcasted_iota(jnp.int32, (8, heads), 0)
    known = jnp.where(each == 0, bias[...].reshape(1, heads), jnp.where(each == 1, rate, 0.0))
    spread = sum(dot(piece, expand[0:heads, :]) for piece in parts_of(known, 3))
    bias_e, rate_e = spread[0:1], spread[1:2]
    taps_v, taps_k, taps_q = (c[...].astype(F32) for c in (cv, ck, cq))
    gain_out = ogain[...].reshape(1, width)
    loads["states"].wait()
    for j in range(own):
        start = states[j, acc_ref[j]]
        start_v[j] = start
        start = start.reshape(width, STATE)
        hi, lo = parts_of(start, 2)
        shi[j] = hi
        slo[j] = lo

    for copy in first:
        copy.wait()
    t_at = lax.broadcasted_iota(jnp.int32, (prop, width), 0)
    results = []
    for j in range(own):
        mine = kv * own + j
        total = own1[mine]
        sums = total[:, 0:conv_cols]
        stats = total[:, conv_cols:conv_cols + LANES]
        for d in range(n_kv - 1):
            got = recv1[d, j].astype(F32)
            sums = sums + got[:, 0:conv_cols]
            stats = stats + got[:, conv_cols:conv_cols + LANES] + got[:, conv_cols + LANES:]
        rscale = lax.rsqrt(stats[:, heads:heads + 1] / (feat * n_kv) + EPS)
        raw = stats[:, 0:heads] * rscale
        raw_e = sum(dot(piece, expand[0:heads, :]) for piece in parts_of(raw, 3))
        hist_ref[j, span:span + prop, :] = (sums * rscale).astype(BF16).astype(F32)

        def conv(c, at, n):
            total = hist_ref[j, 0:prop, at:at + n] * c[0:1]
            for i in range(1, taps):
                total = total + hist_ref[j, i:i + prop, at:at + n] * c[i:i + 1]
            return silu(total)

        conv_k = conv(taps_k, width, kwidth)
        conv_q = conv(taps_q, width + kwidth, kwidth)
        conv_v = conv(taps_v, 0, width)
        pre = raw_e + bias_e
        dt = jnp.maximum(pre, 0.0) + jnp.log1p(jnp.exp(-jnp.abs(pre)))
        logd = dt * rate_e
        moved = dt * conv_v
        chain[j, 0:prop, :] = moved
        chain[j, prop:2 * prop, :] = jnp.exp(logd)
        convk[j] = conv_k
        cum = jnp.zeros_like(logd)
        for s in range(prop):
            cum = cum + jnp.where(t_at >= s, logd[s:s + 1], 0.0)
        parts = []
        for g in range(groups):
            qg = conv_q[:, g * STATE:(g + 1) * STATE]
            kg = conv_k[:, g * STATE:(g + 1) * STATE]
            q_hi, q_lo = parts_of(qg, 2)
            s_hi = shi[j, g * gwidth:(g + 1) * gwidth, :]
            s_lo = slo[j, g * gwidth:(g + 1) * gwidth, :]
            read = functools.partial(lax.dot_general, dimension_numbers=COMMON, preferred_element_type=F32)
            y = read(q_hi, s_hi) + read(q_lo, s_hi) + read(q_hi, s_lo)
            lo_at = g * gwidth
            cum_g = cum[:, lo_at:lo_at + gwidth]
            y = y * jnp.exp(cum_g)
            for s in range(prop):
                kq = jnp.sum(qg * kg[s:s + 1], axis=1, keepdims=True)
                weight = jnp.exp(jnp.where(t_at[:, 0:gwidth] >= s, cum_g - cum_g[s:s + 1], -jnp.inf))
                y = y + weight * (moved[s:s + 1, lo_at:lo_at + gwidth] * kq)
            parts.append(y)
        results.append((jnp.concatenate(parts, axis=1), rscale))

    for copy in second:
        copy.wait()
    for j in range(own):
        mine = kv * own + j
        y, rscale = results[j]
        total = own2[mine]
        for d in range(n_kv - 1):
            total = total + recv2[d, j].astype(F32)
        gate = (total * rscale).astype(BF16).astype(F32)
        gated = y * silu(gate)
        sq_hi, sq_lo = parts_of(jnp.broadcast_to(jnp.sum(gated * gated, axis=1, keepdims=True), (prop, LANES)), 2)
        gbuf[mine, :, 0:width] = (gated * gain_out).astype(BF16)
        gbuf[mine, :, width:width + LANES] = sq_hi
        gbuf[mine, :, width + LANES:] = sq_lo

    gathers = []
    for d in range(1, n_kv):
        peer = lax.rem(kv + d, n_kv)
        gathers.append(pltpu.make_async_remote_copy(
            src_ref=gbuf.at[pl.ds(kv * own, own)], dst_ref=gbuf.at[pl.ds(kv * own, own)],
            send_sem=s3.at[d - 1], recv_sem=r3.at[d - 1],
            device_id={"kv": peer}, device_id_type=MESH))
    for i in sorted(range(n_kv - 1), key=lambda i: -min(i + 1, n_kv - 1 - i)):
        gathers[i].start()
    stores = [pltpu.make_async_copy(src, dst, out_sem.at[i]) for i, (src, dst) in enumerate(
        ((start_v, start_h), (hist_ref, hist_h), (chain, chain_h), (convk, convk_h)))]
    for store in stores:
        store.start()
    loads["wo"].wait()
    for i, copy in enumerate(gathers):
        copy.wait()
    for s in range(n_seq):
        rows_g[s * prop:(s + 1) * prop, :] = gbuf[s].astype(F32)
    outn = rows_g[:, 0:width].astype(BF16)
    psend[:, 0:cols] = dot(outn, wo[...]).astype(BF16)
    psend[:, pcols:pcols + LANES] = rows_g[:, width:width + LANES].astype(BF16)
    psend[:, pcols + LANES:] = rows_g[:, width + LANES:].astype(BF16)
    swaps = []
    for d in range(1, n_tp):
        swaps.append(pltpu.make_async_remote_copy(
            src_ref=psend, dst_ref=precv.at[d - 1], send_sem=s4.at[d - 1], recv_sem=r4.at[d - 1],
            device_id={"tp": lax.rem(tp + d, n_tp)}, device_id_type=MESH))
        swaps[-1].start()
    total = psend[:, 0:cols].astype(F32)
    square = rows_g[:, width:width + 1] + rows_g[:, width + LANES:width + LANES + 1]
    for d, copy in enumerate(swaps):
        copy.wait()
        total = total + precv[d, :, 0:cols].astype(F32)
        square = square + precv[d, :, pcols:pcols + 1].astype(F32)
        square = square + precv[d, :, pcols + LANES:pcols + LANES + 1].astype(F32)
    mixed = total * lax.rsqrt(square / (width * n_tp) + EPS)
    for s in range(n_seq):
        mixed_ref[s] = mixed[s * prop:(s + 1) * prop].astype(BF16)
    for store in stores:
        store.wait()


def states_kernel(chunk, mixed_h, hist_h, chain_h, convk_h, start_h,
                  mixed_ref, new_h, nv_ref, nk_ref, nq_ref,
                  mixed, hist, chain, convk, buf, cols_t, in_sem, load_sem, out_sem):
    own, keep, heads, head_dim, state = buf.shape
    steps = keep - 1
    per_group = heads // (convk.shape[2] // state)
    chunks = heads // chunk
    small = [pltpu.make_async_copy(src, dst, in_sem.at[i]) for i, (src, dst) in enumerate(
        ((chain_h, chain), (convk_h, convk), (hist_h, hist), (mixed_h, mixed)))]
    loads = [[pltpu.make_async_copy(
        start_h.at[j, pl.ds(c * chunk, chunk)], buf.at[j, 0, pl.ds(c * chunk, chunk)],
        load_sem.at[j, c]) for c in range(chunks)] for j in range(own)]
    for copy in small[:2]:
        copy.start()
    for j in range(own):
        for c in range(chunks):
            loads[j][c].start()
    for copy in small[2:]:
        copy.start()
    for copy in small[:2]:
        copy.wait()
    stores = []
    for j in range(own):
        cols_t[...] = jnp.transpose(chain[j])
        for c in range(chunks):
            loads[j][c].wait()
            for h in range(c * chunk, (c + 1) * chunk):
                s = buf[j, 0, h]
                g = h // per_group
                at = h * head_dim
                for t in range(steps):
                    lift = cols_t[at:at + head_dim, t:t + 1]
                    fade = cols_t[at:at + 1, steps + t:steps + t + 1]
                    s = s * fade + lift * convk[j, t:t + 1, g * state:(g + 1) * state]
                    buf[j, t + 1, h] = s
            out = pltpu.make_async_copy(
                buf.at[j, :, pl.ds(c * chunk, chunk)], new_h.at[j, :, pl.ds(c * chunk, chunk)], out_sem.at[j, c])
            out.start()
            stores.append(out)
    for copy in small[2:]:
        copy.wait()
    mixed_ref[...] = mixed[...]
    at = 0
    for ref in (nv_ref, nk_ref, nq_ref):
        n = ref.shape[2]
        for j in range(own):
            ref[j] = hist[j, 0:ref.shape[1], at:at + n].astype(BF16)
        at += n
    for out in stores:
        out.wait()


def per_device(n_kv, n_tp, *args):
    (tokens, in_gain, w_gate, w_value, w_key, w_query, w_step, conv_value, conv_key, conv_query, step_bias,
     decay_log, out_gain, w_out, past_value, past_key, past_query, past_states, accepted) = args
    n_seq, prop, feat = tokens.shape
    own, keep, heads, head_dim, state = past_states.shape
    width, kwidth, cols = w_value.shape[1], w_key.shape[1], w_out.shape[1]
    conv_cols = width + 2 * kwidth
    wide1 = conv_cols + 2 * LANES
    gcols = width + 2 * LANES
    pcols = -(-cols // LANES) * LANES + 2 * LANES
    rows = n_seq * prop
    hist_rows = past_value.shape[1]
    vmem = pl.BlockSpec(memory_space=pltpu.VMEM)
    hbm = pl.BlockSpec(memory_space=pltpu.HBM)
    dma = pltpu.SemaphoreType.DMA
    args = args[:6] + (w_step.T,) + args[7:]
    held = [pltpu.VMEM(a.shape, a.dtype) for a in args[:-1]] + [pltpu.SMEM(accepted.shape, accepted.dtype)]
    peers = n_kv - 1
    passed = (
        jax.ShapeDtypeStruct((n_seq, prop, cols), BF16),
        jax.ShapeDtypeStruct((own, hist_rows, conv_cols), F32),
        jax.ShapeDtypeStruct((own, 2 * prop, width), F32),
        jax.ShapeDtypeStruct((own, prop, kwidth), F32),
        jax.ShapeDtypeStruct((own, heads, head_dim, state), F32),
    )
    kept = [pltpu.VMEM(a.shape, a.dtype) for a in passed]
    handed = pl.pallas_call(
        functools.partial(mixer_kernel, n_kv, n_tp),
        out_shape=passed,
        in_specs=[hbm] * 19,
        out_specs=(vmem,) + (hbm,) * 4,
        scratch_shapes=held + [
            pltpu.VMEM((rows, feat), F32),
            pltpu.VMEM((n_seq, prop, wide1), BF16),
            pltpu.VMEM((peers, own, prop, wide1), BF16),
            pltpu.VMEM((n_seq, prop, conv_cols + LANES), F32),
            pltpu.VMEM((n_seq, prop, width), BF16),
            pltpu.VMEM((peers, own, prop, width), BF16),
            pltpu.VMEM((n_seq, prop, width), F32),
            pltpu.VMEM((LANES, width), BF16),
            pltpu.VMEM((own, width, state), BF16),
            pltpu.VMEM((own, width, state), BF16),
            pltpu.VMEM((n_seq, prop, gcols), BF16),
            pltpu.VMEM((rows, gcols), F32),
            pltpu.VMEM((rows, pcols), BF16),
            pltpu.VMEM((n_tp - 1, rows, pcols), BF16),
        ] + kept[1:] + [
            dma((19,)), dma((4,)),
            dma((peers,)), dma((peers,)), dma((peers,)), dma((peers,)), dma((peers,)), dma((peers,)),
            dma((n_tp - 1,)), dma((n_tp - 1,)),
        ],
        compiler_params=pltpu.CompilerParams(
            collective_id=0, has_side_effects=True, vmem_limit_bytes=VMEM_BYTES),
        name="mixer",
    )(*args)
    chunk = 4 if heads % 4 == 0 else 1
    mixed, new_states, new_value, new_key, new_query = pl.pallas_call(
        functools.partial(states_kernel, chunk),
        out_shape=passed[:1] + tuple(
            jax.ShapeDtypeStruct(a.shape, a.dtype) for a in (past_states, past_value, past_key, past_query)),
        in_specs=[hbm] * 5,
        out_specs=(vmem, hbm, vmem, vmem, vmem),
        scratch_shapes=kept[:4] + [
            pltpu.VMEM(past_states.shape, F32),
            pltpu.VMEM((width, 2 * prop), F32),
            dma((4,)), dma((own, heads // chunk)), dma((own, heads // chunk)),
        ],
        compiler_params=pltpu.CompilerParams(vmem_limit_bytes=VMEM_BYTES),
        name="states",
    )(*handed)
    return (mixed, new_states, new_value, new_key, new_query)


def solution(mesh):
    seqs = ("dp", "kv")
    placed = (
        P("dp", None, "kv"), P("kv"),
        P("kv", "tp"), P("kv", "tp"), P("kv", "tp"), P("kv", "tp"), P("kv", "tp"),
        P(None, "tp"), P(None, "tp"), P(None, "tp"),
        P("tp"), P("tp"), P("tp"), P("tp", "kv"),
        P(seqs, None, "tp"), P(seqs, None, "tp"), P(seqs, None, "tp"),
        P(seqs, None, "tp", None, None), P(seqs),
    )
    return jax.shard_map(
        functools.partial(per_device, mesh.shape["kv"], mesh.shape["tp"]),
        mesh=mesh,
        in_specs=placed,
        out_specs=(
            P("dp", None, "kv"),
            P(seqs, None, "tp", None, None),
            P(seqs, None, "tp"), P(seqs, None, "tp"), P(seqs, None, "tp"),
        ),
        check_vma=False,
    )
```

```python
import functools

import jax
import jax.numpy as jnp
from jax import lax
from jax.experimental import pallas as pl
from jax.experimental.pallas import tpu as pltpu
from jax.sharding import PartitionSpec as P

STATE = 128
EPS = 1e-05
LANES = 128
HALF = LANES // 2
VMEM_BYTES = 67043328
MESH = pl.DeviceIdType.MESH
F32 = jnp.float32
BF16 = jnp.bfloat16
COMMON = (((1,), (1,)), ((), ()))


def parts_of(x, count):
    found = []
    for _ in range(count):
        piece = x.astype(BF16)
        found.append(piece)
        x = x - piece.astype(F32)
    return found


def silu(x):
    return x / (1.0 + jnp.exp(-x))


def dot(a, b):
    return jnp.dot(a, b, preferred_element_type=F32)


def mixer_kernel(n_kv, n_tp, *refs):
    (tok_h, gain_h, wg_h, wv_h, wk_h, wq_h, ws_h, cv_h, ck_h, cq_h, bias_h, dlog_h, ogain_h, wo_h,
     pv_h, pk_h, pq_h, states_h, acc_h,
     mixed_ref, hist_h, chain_h, convk_h, start_h,
     tok, gain, wg, wv, wk, wq, ws, cv, ck, cq, bias, dlog, ogain, wo, pv, pk, pq, states, acc_ref,
     rows_f, send1, recv1, own1, send2, recv2, own2, expand, shi, slo, gbuf, rows_g, psend, precv, hist_ref, chain, convk, start_v,
     load_sem, out_sem, s1, r1, s2, r2, s3, r3, s4, r4) = refs
    kv = lax.axis_index("kv")
    tp = lax.axis_index("tp")
    n_seq, prop, feat = tok.shape
    own = pv.shape[0]
    rows = n_seq * prop
    width, kwidth, heads = wv.shape[1], wk.shape[1], ws.shape[0]
    head_dim = width // heads
    groups = kwidth // STATE
    gwidth = width // groups
    taps = cv.shape[0]
    cols = wo.shape[1]
    pcols = psend.shape[1] - LANES
    conv_cols = width + 2 * kwidth

    barrier = pltpu.get_barrier_semaphore()
    for d in range(1, n_kv):
        pl.semaphore_signal(barrier, inc=1, device_id={"kv": lax.rem(kv + d, n_kv)}, device_id_type=MESH)
    for d in range(1, n_tp):
        pl.semaphore_signal(barrier, inc=1, device_id={"tp": lax.rem(tp + d, n_tp)}, device_id_type=MESH)

    pairs = dict(
        tok=(tok_h, tok), gain=(gain_h, gain), ws=(ws_h, ws), wk=(wk_h, wk), wq=(wq_h, wq), wv=(wv_h, wv),
        wg=(wg_h, wg), pv=(pv_h, pv), pk=(pk_h, pk), pq=(pq_h, pq), cv=(cv_h, cv), ck=(ck_h, ck), cq=(cq_h, cq),
        bias=(bias_h, bias), dlog=(dlog_h, dlog), ogain=(ogain_h, ogain), states=(states_h, states), wo=(wo_h, wo), acc=(acc_h, acc_ref),
    )
    loads = {}
    for place, (name, (src, dst)) in enumerate(pairs.items()):
        loads[name] = pltpu.make_async_copy(src, dst, load_sem.at[place])
        loads[name].start()

    row_at = lax.broadcasted_iota(jnp.int32, (LANES, width), 0)
    col_at = lax.broadcasted_iota(jnp.int32, (LANES, width), 1)
    expand[...] = jnp.where(row_at == col_at // head_dim, 1.0, 0.0).astype(BF16)
    lane = lax.broadcasted_iota(jnp.int32, (rows, LANES), 1)

    loads["tok"].wait()
    loads["gain"].wait()
    for s in range(n_seq):
        rows_f[s * prop:(s + 1) * prop, :] = tok[s].astype(F32)
    x = rows_f[...]
    normed = (x * gain[...].reshape(1, feat)).astype(BF16)
    squares = jnp.sum(x * x, axis=1, keepdims=True)

    def stage(product, send, kept, at):
        n = product.shape[1]
        for s in range(n_seq):
            piece = product[s * prop:(s + 1) * prop]
            kept[s, :, at:at + n] = piece
            send[s, :, at:at + n] = piece.astype(BF16)

    loads["ws"].wait()
    step_part = lax.dot_general(normed, ws[...], COMMON, preferred_element_type=F32)
    rows_g[:, 0:LANES] = jnp.zeros((rows, LANES), F32)
    rows_g[:, 0:heads] = step_part
    stat = jnp.where(lane == heads, squares, rows_g[:, 0:LANES])
    stat_hi = stat.astype(BF16).astype(F32)
    packed = stat_hi + pltpu.roll(stat - stat_hi, HALF, 1)
    for s in range(n_seq):
        own1[s, :, conv_cols:] = stat[s * prop:(s + 1) * prop]
        send1[s, :, conv_cols:] = packed[s * prop:(s + 1) * prop].astype(BF16)
    loads["wk"].wait()
    stage(dot(normed, wk[...]), send1, own1, width)
    loads["wq"].wait()
    stage(dot(normed, wq[...]), send1, own1, width + kwidth)
    loads["wv"].wait()
    stage(dot(normed, wv[...]), send1, own1, 0)

    pl.semaphore_wait(barrier, n_kv - 1 + n_tp - 1)

    def scatter(send, recv, send_sem, recv_sem):
        copies = []
        for d in range(1, n_kv):
            peer = lax.rem(kv + d, n_kv)
            copies.append(pltpu.make_async_remote_copy(
                src_ref=send.at[pl.ds(peer * own, own)], dst_ref=recv.at[d - 1],
                send_sem=send_sem.at[d - 1], recv_sem=recv_sem.at[d - 1],
                device_id={"kv": peer}, device_id_type=MESH))
        order = sorted(range(n_kv - 1), key=lambda i: -min(i + 1, n_kv - 1 - i))
        for i in order:
            copies[i].start()
        return copies

    first = scatter(send1, recv1, s1, r1)
    loads["wg"].wait()
    stage(dot(normed, wg[...]), send2, own2, 0)
    second = scatter(send2, recv2, s2, r2)

    for name in ("acc", "pv", "pk", "pq", "cv", "ck", "cq", "bias", "dlog", "ogain"):
        loads[name].wait()
    span = taps - 1
    for j in range(own):
        chosen = acc_ref[j]
        at = 0
        for past in (pv, pk, pq):
            wide = past[j].astype(F32)
            window = wide[0:span]
            for a in range(1, wide.shape[0] - span + 1):
                window = jnp.where(chosen == a, wide[a:a + span], window)
            hist_ref[j, 0:span, at:at + wide.shape[1]] = window
            at += wide.shape[1]
    rate = -jnp.exp(dlog[...].reshape(1, heads))
    each = lax.broadcasted_iota(jnp.int32, (8, heads), 0)
    known = jnp.where(each == 0, bias[...].reshape(1, heads), jnp.where(each == 1, rate, 0.0))
    spread = sum(dot(piece, expand[0:heads, :]) for piece in parts_of(known, 3))
    bias_e, rate_e = spread[0:1], spread[1:2]
    taps_v, taps_k, taps_q = (c[...].astype(F32) for c in (cv, ck, cq))
    gain_out = ogain[...].reshape(1, width)
    loads["states"].wait()
    for j in range(own):
        start = states[j, acc_ref[j]]
        start_v[j] = start
        start = start.reshape(width, STATE)
        hi, lo = parts_of(start, 2)
        shi[j] = hi
        slo[j] = lo

    for copy in first:
        copy.wait()
    t_at = lax.broadcasted_iota(jnp.int32, (prop, width), 0)
    results = []
    for j in range(own):
        mine = kv * own + j
        total = own1[mine]
        sums = total[:, 0:conv_cols]
        stats = total[:, conv_cols:]
        for d in range(n_kv - 1):
            got = recv1[d, j].astype(F32)
            sums = sums + got[:, 0:conv_cols]
            stats = stats + got[:, conv_cols:] + pltpu.roll(got[:, conv_cols:], HALF, 1)
        rscale = lax.rsqrt(stats[:, heads:heads + 1] / (feat * n_kv) + EPS)
        raw = stats[:, 0:heads] * rscale
        raw_e = sum(dot(piece, expand[0:heads, :]) for piece in parts_of(raw, 3))
        hist_ref[j, span:span + prop, :] = (sums * rscale).astype(BF16).astype(F32)

        def conv(c, at, n):
            total = hist_ref[j, 0:prop, at:at + n] * c[0:1]
            for i in range(1, taps):
                total = total + hist_ref[j, i:i + prop, at:at + n] * c[i:i + 1]
            return silu(total)

        conv_k = conv(taps_k, width, kwidth)
        conv_q = conv(taps_q, width + kwidth, kwidth)
        conv_v = conv(taps_v, 0, width)
        pre = raw_e + bias_e
        dt = jnp.maximum(pre, 0.0) + jnp.log1p(jnp.exp(-jnp.abs(pre)))
        logd = dt * rate_e
        moved = dt * conv_v
        chain[j, 0:prop, :] = moved
        chain[j, prop:2 * prop, :] = jnp.exp(logd)
        convk[j] = conv_k
        cum = jnp.zeros_like(logd)
        for s in range(prop):
            cum = cum + jnp.where(t_at >= s, logd[s:s + 1], 0.0)
        parts = []
        for g in range(groups):
            qg = conv_q[:, g * STATE:(g + 1) * STATE]
            kg = conv_k[:, g * STATE:(g + 1) * STATE]
            q_hi, q_lo = parts_of(qg, 2)
            s_hi = shi[j, g * gwidth:(g + 1) * gwidth, :]
            s_lo = slo[j, g * gwidth:(g + 1) * gwidth, :]
            read = functools.partial(lax.dot_general, dimension_numbers=COMMON, preferred_element_type=F32)
            y = read(q_hi, s_hi) + read(q_lo, s_hi) + read(q_hi, s_lo)
            lo_at = g * gwidth
            cum_g = cum[:, lo_at:lo_at + gwidth]
            y = y * jnp.exp(cum_g)
            for s in range(prop):
                kq = jnp.sum(qg * kg[s:s + 1], axis=1, keepdims=True)
                weight = jnp.exp(jnp.where(t_at[:, 0:gwidth] >= s, cum_g - cum_g[s:s + 1], -jnp.inf))
                y = y + weight * (moved[s:s + 1, lo_at:lo_at + gwidth] * kq)
            parts.append(y)
        results.append((jnp.concatenate(parts, axis=1), rscale))

    for copy in second:
        copy.wait()
    for j in range(own):
        mine = kv * own + j
        y, rscale = results[j]
        total = own2[mine]
        for d in range(n_kv - 1):
            total = total + recv2[d, j].astype(F32)
        gate = (total * rscale).astype(BF16).astype(F32)
        gated = y * silu(gate)
        square = jnp.sum(gated * gated, axis=1, keepdims=True)
        square_hi = square.astype(BF16).astype(F32)
        gbuf[mine, :, 0:width] = (gated * gain_out).astype(BF16)
        gbuf[mine, :, width:] = jnp.where(lane[0:prop] == 0, square_hi, square - square_hi).astype(BF16)

    gathers = []
    for d in range(1, n_kv):
        peer = lax.rem(kv + d, n_kv)
        gathers.append(pltpu.make_async_remote_copy(
            src_ref=gbuf.at[pl.ds(kv * own, own)], dst_ref=gbuf.at[pl.ds(kv * own, own)],
            send_sem=s3.at[d - 1], recv_sem=r3.at[d - 1],
            device_id={"kv": peer}, device_id_type=MESH))
    for i in sorted(range(n_kv - 1), key=lambda i: -min(i + 1, n_kv - 1 - i)):
        gathers[i].start()
    stores = [pltpu.make_async_copy(src, dst, out_sem.at[i]) for i, (src, dst) in enumerate(
        ((start_v, start_h), (hist_ref, hist_h), (chain, chain_h), (convk, convk_h)))]
    for store in stores:
        store.start()
    loads["wo"].wait()
    for i, copy in enumerate(gathers):
        copy.wait()
    for s in range(n_seq):
        rows_g[s * prop:(s + 1) * prop, :] = gbuf[s].astype(F32)
    outn = rows_g[:, 0:width].astype(BF16)
    psend[:, 0:cols] = dot(outn, wo[...]).astype(BF16)
    psend[:, pcols:] = rows_g[:, width:].astype(BF16)
    swaps = []
    for d in range(1, n_tp):
        swaps.append(pltpu.make_async_remote_copy(
            src_ref=psend, dst_ref=precv.at[d - 1], send_sem=s4.at[d - 1], recv_sem=r4.at[d - 1],
            device_id={"tp": lax.rem(tp + d, n_tp)}, device_id_type=MESH))
        swaps[-1].start()
    total = psend[:, 0:cols].astype(F32)
    square = rows_g[:, width:width + 1] + rows_g[:, width + 1:width + 2]
    for d, copy in enumerate(swaps):
        copy.wait()
        total = total + precv[d, :, 0:cols].astype(F32)
        extra = precv[d, :, pcols:].astype(F32)
        square = square + extra[:, 0:1] + extra[:, 1:2]
    mixed = total * lax.rsqrt(square / (width * n_tp) + EPS)
    for s in range(n_seq):
        mixed_ref[s] = mixed[s * prop:(s + 1) * prop].astype(BF16)
    for store in stores:
        store.wait()


def states_kernel(chunk, mixed_h, hist_h, chain_h, convk_h, start_h,
                  mixed_out, new_h, nv_h, nk_h, nq_h,
                  mixed, hist, chain, convk, buf, cols_t, nv, nk, nq, in_sem, load_sem, out_sem, end_sem):
    own, keep, heads, head_dim, state = buf.shape
    steps = keep - 1
    per_group = heads // (convk.shape[2] // state)
    chunks = heads // chunk
    small = [pltpu.make_async_copy(src, dst, in_sem.at[i]) for i, (src, dst) in enumerate(
        ((chain_h, chain), (convk_h, convk), (hist_h, hist), (mixed_h, mixed)))]
    loads = [[pltpu.make_async_copy(
        start_h.at[j, pl.ds(c * chunk, chunk)], buf.at[j, 0, pl.ds(c * chunk, chunk)],
        load_sem.at[j, c]) for c in range(chunks)] for j in range(own)]
    for copy in small[:2]:
        copy.start()
    for j in range(own):
        for c in range(chunks):
            loads[j][c].start()
    for copy in small[2:]:
        copy.start()
    for copy in small[:2]:
        copy.wait()
    stores, ends = [], []
    for j in range(own):
        cols_t[...] = jnp.transpose(chain[j])
        for c in range(chunks):
            loads[j][c].wait()
            for h in range(c * chunk, (c + 1) * chunk):
                s = buf[j, 0, h]
                g = h // per_group
                at = h * head_dim
                for t in range(steps):
                    lift = cols_t[at:at + head_dim, t:t + 1]
                    fade = cols_t[at:at + 1, steps + t:steps + t + 1]
                    s = s * fade + lift * convk[j, t:t + 1, g * state:(g + 1) * state]
                    buf[j, t + 1, h] = s
            out = pltpu.make_async_copy(
                buf.at[j, :, pl.ds(c * chunk, chunk)], new_h.at[j, :, pl.ds(c * chunk, chunk)], out_sem.at[j, c])
            out.start()
            stores.append(out)
            if not ends:
                for copy in small[2:]:
                    copy.wait()
                at = 0
                for ref in (nv, nk, nq):
                    n = ref.shape[2]
                    for i in range(own):
                        ref[i] = hist[i, 0:ref.shape[1], at:at + n].astype(BF16)
                    at += n
                ends = [pltpu.make_async_copy(src, dst, end_sem.at[i]) for i, (src, dst) in enumerate(
                    ((mixed, mixed_out), (nv, nv_h), (nk, nk_h), (nq, nq_h)))]
                for end in ends:
                    end.start()
    for out in stores + ends:
        out.wait()


def per_device(n_kv, n_tp, *args):
    (tokens, in_gain, w_gate, w_value, w_key, w_query, w_step, conv_value, conv_key, conv_query, step_bias,
     decay_log, out_gain, w_out, past_value, past_key, past_query, past_states, accepted) = args
    n_seq, prop, feat = tokens.shape
    own, keep, heads, head_dim, state = past_states.shape
    width, kwidth, cols = w_value.shape[1], w_key.shape[1], w_out.shape[1]
    conv_cols = width + 2 * kwidth
    wide1 = conv_cols + LANES
    gcols = width + LANES
    pcols = -(-cols // LANES) * LANES + LANES
    rows = n_seq * prop
    hist_rows = past_value.shape[1]
    vmem = pl.BlockSpec(memory_space=pltpu.VMEM)
    hbm = pl.BlockSpec(memory_space=pltpu.HBM)
    dma = pltpu.SemaphoreType.DMA
    args = args[:6] + (w_step.T,) + args[7:]
    held = [pltpu.VMEM(a.shape, a.dtype) for a in args[:-1]] + [pltpu.SMEM(accepted.shape, accepted.dtype)]
    peers = n_kv - 1
    passed = (
        jax.ShapeDtypeStruct((n_seq, prop, cols), BF16),
        jax.ShapeDtypeStruct((own, hist_rows, conv_cols), F32),
        jax.ShapeDtypeStruct((own, 2 * prop, width), F32),
        jax.ShapeDtypeStruct((own, prop, kwidth), F32),
        jax.ShapeDtypeStruct((own, heads, head_dim, state), F32),
    )
    kept = [pltpu.VMEM(a.shape, a.dtype) for a in passed]
    handed = pl.pallas_call(
        functools.partial(mixer_kernel, n_kv, n_tp),
        out_shape=passed,
        in_specs=[hbm] * 19,
        out_specs=(vmem,) + (hbm,) * 4,
        scratch_shapes=held + [
            pltpu.VMEM((rows, feat), F32),
            pltpu.VMEM((n_seq, prop, wide1), BF16),
            pltpu.VMEM((peers, own, prop, wide1), BF16),
            pltpu.VMEM((n_seq, prop, conv_cols + LANES), F32),
            pltpu.VMEM((n_seq, prop, width), BF16),
            pltpu.VMEM((peers, own, prop, width), BF16),
            pltpu.VMEM((n_seq, prop, width), F32),
            pltpu.VMEM((LANES, width), BF16),
            pltpu.VMEM((own, width, state), BF16),
            pltpu.VMEM((own, width, state), BF16),
            pltpu.VMEM((n_seq, prop, gcols), BF16),
            pltpu.VMEM((rows, gcols), F32),
            pltpu.VMEM((rows, pcols), BF16),
            pltpu.VMEM((n_tp - 1, rows, pcols), BF16),
        ] + kept[1:] + [
            dma((19,)), dma((4,)),
            dma((peers,)), dma((peers,)), dma((peers,)), dma((peers,)), dma((peers,)), dma((peers,)),
            dma((n_tp - 1,)), dma((n_tp - 1,)),
        ],
        compiler_params=pltpu.CompilerParams(
            collective_id=0, has_side_effects=True, vmem_limit_bytes=VMEM_BYTES),
        name="mixer",
    )(*args)
    chunk = 4 if heads % 4 == 0 else 1
    mixed, new_states, new_value, new_key, new_query = pl.pallas_call(
        functools.partial(states_kernel, chunk),
        out_shape=passed[:1] + tuple(
            jax.ShapeDtypeStruct(a.shape, a.dtype) for a in (past_states, past_value, past_key, past_query)),
        in_specs=[hbm] * 5,
        out_specs=(hbm,) * 5,
        scratch_shapes=kept[:4] + [
            pltpu.VMEM(past_states.shape, F32),
            pltpu.VMEM((width, 2 * prop), F32),
            pltpu.VMEM(past_value.shape, BF16), pltpu.VMEM(past_key.shape, BF16), pltpu.VMEM(past_query.shape, BF16),
            dma((4,)), dma((own, heads // chunk)), dma((own, heads // chunk)), dma((4,)),
        ],
        compiler_params=pltpu.CompilerParams(vmem_limit_bytes=VMEM_BYTES),
        name="states",
    )(*handed)
    return (mixed, new_states, new_value, new_key, new_query)


def solution(mesh):
    seqs = ("dp", "kv")
    placed = (
        P("dp", None, "kv"), P("kv"),
        P("kv", "tp"), P("kv", "tp"), P("kv", "tp"), P("kv", "tp"), P("kv", "tp"),
        P(None, "tp"), P(None, "tp"), P(None, "tp"),
        P("tp"), P("tp"), P("tp"), P("tp", "kv"),
        P(seqs, None, "tp"), P(seqs, None, "tp"), P(seqs, None, "tp"),
        P(seqs, None, "tp", None, None), P(seqs),
    )
    return jax.shard_map(
        functools.partial(per_device, mesh.shape["kv"], mesh.shape["tp"]),
        mesh=mesh,
        in_specs=placed,
        out_specs=(
            P("dp", None, "kv"),
            P(seqs, None, "tp", None, None),
            P(seqs, None, "tp"), P(seqs, None, "tp"), P(seqs, None, "tp"),
        ),
        check_vma=False,
    )
```
